1024 devices in a mesh: ep: 64 (over z, y), tp: 16 (over x, core).
Axes of the slice: x: 8, y: 8, z: 8, core: 2. Of those that a mesh axis runs over, the one named last changes fastest.
Arguments:
- tokens: bfloat16 [10752, 2048], P('ep'), may hold values from -6 to 6
- cotangent: bfloat16 [10752, 2048], P('ep'), may hold values from -6 to 6
- group_ids: int32 [10752, 1], P('ep'), may hold values from 0 to 63; in each aligned block of 168 rows (0 to 167, 168 to 335, ...) at most 4 rows name the same one
- within_ids: int32 [10752, 2], P('ep'), may hold values from 0 to 1, all different within a row
- gate_weights: bfloat16 [10752, 2], P('ep'), may hold values from 0.099609375 to 1
- w_gate: bfloat16 [128, 2048, 1024], P('ep', None, 'tp'), may hold values from -0.125 to 0.125
- w_up: bfloat16 [128, 2048, 1024], P('ep', None, 'tp'), may hold values from -0.125 to 0.125
- w_down: bfloat16 [128, 1024, 2048], P('ep', 'tp'), may hold values from -0.1875 to 0.1875
Outputs:
- tokens_grad: bfloat16 [10752, 2048], P('ep', 'tp')
- gate_grad: float32 [10752, 2], P('ep')
- w_gate_grad: bfloat16 [128, 2048, 1024], P('ep', None, 'tp')
- w_up_grad: bfloat16 [128, 2048, 1024], P('ep', None, 'tp')
- w_down_grad: bfloat16 [128, 1024, 2048], P('ep', 'tp')
The draws below stay inside these ranges and needn't reach their ends.
Inputs may be any that keep to these rules, and one draw needn't show every extreme that they name: `group_ids`: in the rows of one device no group is chosen by more than 4 rows. `within_ids`: the two entries of a row differ.
All inputs are finite; a program needn't handle non-finite values.
Results may differ from the reference program's by a relative error of at most 0.017.
Values may be sent and summed in bfloat16 or wider, within the bound.
No kernel may reach another device: no remote copies, remote signals or barrier semaphores. Data moves between devices by JAX's collectives and lax.ppermute only.
A program may use at most 64 MiB of HBM per device.

```python
import math
import jax
import jax.numpy as jnp
import numpy as np
from jax import lax

D = 2048
FF = 1024
GROUP_EXPERTS = 2
TOP_K = 2
TOK_DEV = 168
GROUPS = 64
EXPERTS = 128
CAP = 4
TOKENS = 10752
N_EP = 64
N_TP = 16


def steps_of(stream_key, shape, shards, least, largest):
    loudness, own = 1.0, jax.random.fold_in(stream_key, 6)
    for position, shards_of in shards:
        steps = jnp.exp(jax.random.uniform(jax.random.fold_in(own, position), (shards_of,), jnp.float32, least / len(shards), largest / len(shards)))
        loudness = loudness * jnp.repeat(steps, shape[position] // shards_of).reshape([-1 if axis == position else 1 for axis in range(len(shape))])
    return loudness


def different_ones(stream_key, rows, number_of, top, lift):
    ranking = jax.random.permutation(jax.random.fold_in(stream_key, 1), number_of)
    pull = ranking
    for power in range(3):
        pull = pull * pull // number_of
    pull = pull * lift // number_of
    tickets = jax.random.randint(jax.random.fold_in(stream_key, 2), (rows, number_of), 0, 4096) + pull
    sure = jax.random.permutation(jax.random.fold_in(stream_key, 3), rows)[jnp.arange(number_of) % rows]
    tickets = jnp.where(jnp.arange(rows)[:, None] == sure[None, :], 1 << 14, tickets)
    score = tickets * number_of + jnp.arange(number_of)
    return lax.top_k(score.astype(jnp.int32), top)[1].astype(jnp.int32)


def routed_block(rng, own, number, rows, count, top, bound, lean):
    ranking = jax.random.permutation(rng, count)
    packed, usual = portions_of(count, rows * top, bound, lean, True), portions_of(count, rows * top, bound, lean, False)
    places = jnp.arange(count)

    def named(sizes, turn):
        used = int((sizes > 0).sum())
        fixed = max(1, used // 4)
        moved = fixed + (places - fixed + turn * (used - fixed)) % max(1, count - fixed)
        return jnp.zeros((count,), jnp.int32).at[ranking[jnp.where(places < fixed, places, moved)]].set(jnp.asarray(sizes, jnp.int32))

    sizes = jnp.where(number % 4 == 0, named(packed, number // 4), named(usual, number - number // 4 - 1))
    mixed = jax.random.permutation(jax.random.fold_in(own, 3), count)
    source_of, receiver = mixed[0:count // 2 * 2:2], mixed[1:count // 2 * 2:2]
    margin = jnp.minimum(sizes[source_of] - 1, bound - sizes[receiver]) // 2
    margin = jnp.where((source_of == ranking[0]) | (receiver == ranking[0]) | (sizes[receiver] == 0), 0, jnp.maximum(margin, 0))
    moved = jax.random.randint(jax.random.fold_in(own, 4), (count // 2,), 0, 1 << 20) % (margin + 1)
    sizes = sizes.at[source_of].add(-moved).at[receiver].add(moved)
    items = jnp.searchsorted(jnp.cumsum(sizes), jnp.arange(rows * top), side="right").astype(jnp.int32)
    grid = items.reshape(top, rows).T
    grid = grid[jax.random.permutation(jax.random.fold_in(own, 1), rows)]
    turn = jax.random.randint(jax.random.fold_in(own, 2), (rows, 1), 0, top)
    return jnp.take_along_axis(grid, (jnp.arange(top)[None, :] + turn) % top, axis=1)


def portions_of(number_of, total, bound, lean, full):
    loads = [(1 << 20) // math.isqrt(rank ** lean) + 1 for rank in range(1, number_of + 1)]
    largest = bound if full else min(bound, max(-(-total // number_of), total * loads[0] // sum(loads)))
    least = 1 if total - largest >= number_of - 1 else 0
    counts, spare = [largest] + [least] * (number_of - 1), total - largest - least * (number_of - 1)
    while spare > 0:
        free = [i for i in range(1, number_of) if counts[i] < largest] or [i for i in range(1, number_of) if counts[i] < bound]
        mass, remaining = sum([loads[i] for i in free]), spare
        for i in free:
            more = min(bound - counts[i], max(1, remaining * loads[i] // mass), spare)
            counts[i] = counts[i] + more
            spare = spare - more
    return np.array(counts)


def noise(stream_key, dims, spread, bound, pieces=(), kind=jnp.bfloat16):
    gain = steps_of(stream_key, dims, pieces, -0.22, 0.18) if pieces else 1.0
    array = jax.random.normal(stream_key, dims, jnp.float32) * spread * gain
    return jnp.minimum(jnp.maximum(array, -bound), bound).astype(kind)


def setup_inputs(seed: int = 0) -> dict:
    splits = jax.random.split(jax.random.key(seed), 9)
    tokens = noise(splits[0], (TOKENS, D), 1.0, 6.0, ((0, 64),))
    cotangent = noise(splits[1], (TOKENS, D), 1.0, 6.0, ((0, 64),))
    group_ids_keys = jax.random.split(jax.random.fold_in(splits[2], 1), TOKENS // TOK_DEV)
    group_ids_turns = jax.random.permutation(jax.random.fold_in(splits[2], 3), TOKENS // TOK_DEV)
    group_ids = jax.vmap(lambda own, number: routed_block(jax.random.fold_in(splits[2], 2), own, number, TOK_DEV, GROUPS, 1, CAP, 2))(group_ids_keys, group_ids_turns).reshape((TOKENS, 1))
    within_ids = different_ones(splits[3], TOKENS, GROUP_EXPERTS, TOP_K, 8192)
    gate_weights = jnp.clip(jnp.exp(math.log(1.0) - 2.306499 * jax.random.uniform(splits[4], (TOKENS, TOP_K), jnp.float32) ** steps_of(splits[4], (TOKENS, TOP_K), ((0, 64),), -0.2, 0.2)), 0.099609375, 1.0).astype(jnp.bfloat16)
    w_gate = noise(splits[5], (EXPERTS, D, FF), D ** -0.5, 0.125, ((0, 64), (2, 16)))
    w_up = noise(splits[6], (EXPERTS, D, FF), D ** -0.5, 0.125, ((0, 64), (2, 16)))
    w_down = noise(splits[7], (EXPERTS, FF, D), FF ** -0.5, 0.1875, ((0, 64), (1, 16)))
    return {"tokens": tokens, "cotangent": cotangent, "group_ids": group_ids, "within_ids": within_ids, "gate_weights": gate_weights, "w_gate": w_gate, "w_up": w_up, "w_down": w_down}


def reference(tokens, cotangent, group_ids, within_ids, gate_weights, w_gate, w_up, w_down):
    rows_max = N_EP * CAP
    ff_local = FF // N_TP
    group_of = group_ids[:, 0]
    sorted_rows = jnp.argsort(group_of, stable=True).astype(jnp.int32)
    in_group = (group_of[:, None] == jnp.arange(GROUPS, dtype=jnp.int32)[None, :]).astype(jnp.int32)
    group_counts = jnp.sum(in_group, axis=0)
    offsets = jnp.cumsum(group_counts) - group_counts
    local_ids = jnp.arange(GROUP_EXPERTS, dtype=jnp.int32)
    chosen = (within_ids[:, :, None] == local_ids[None, None, :]).astype(jnp.float32)
    combine = jnp.sum(chosen * gate_weights.astype(jnp.float32)[:, :, None], axis=1).astype(jnp.bfloat16)

    def one_group(group_index):
        positions = jnp.arange(rows_max, dtype=jnp.int32)
        is_valid = positions < group_counts[group_index]
        row_ids = sorted_rows[jnp.clip(offsets[group_index] + positions, 0, TOKENS - 1)]
        keep = is_valid[:, None]
        slot_x = jnp.where(keep, tokens[row_ids], jnp.zeros((), jnp.bfloat16))
        slot_dy = jnp.where(keep, cotangent[row_ids], jnp.zeros((), jnp.bfloat16))
        slot_comb = jnp.where(keep, combine[row_ids], jnp.zeros((), jnp.bfloat16))
        first = (group_index * GROUP_EXPERTS).astype(jnp.int32)
        local_gate = lax.dynamic_slice_in_dim(w_gate, first, GROUP_EXPERTS, 0)
        local_up = lax.dynamic_slice_in_dim(w_up, first, GROUP_EXPERTS, 0)
        local_down = lax.dynamic_slice_in_dim(w_down, first, GROUP_EXPERTS, 0)
        dy_float = slot_dy.astype(jnp.float32)
        blocks = jnp.zeros((N_TP, rows_max, D), jnp.float32)
        gate_parts = []
        grads_gate = []
        grads_up = []
        grads_down = []
        for expert in range(GROUP_EXPERTS):
            pre_gate = jnp.dot(slot_x, local_gate[expert], preferred_element_type=jnp.float32)
            pre_up = jnp.dot(slot_x, local_up[expert], preferred_element_type=jnp.float32)
            sig_gate = jax.nn.sigmoid(pre_gate)
            act_b = (pre_gate * sig_gate * pre_up).astype(jnp.bfloat16)
            down = jnp.dot(act_b, local_down[expert], preferred_element_type=jnp.float32)
            gate_parts.append(jnp.sum(dy_float * down, axis=1))
            scaled = (slot_comb[:, expert:expert + 1].astype(jnp.float32) * dy_float).astype(jnp.bfloat16)
            grads_down.append(jnp.dot(act_b.T, scaled, preferred_element_type=jnp.float32).astype(jnp.bfloat16))
            act_grad = jnp.dot(scaled, local_down[expert].T, preferred_element_type=jnp.float32)
            gate_b = (act_grad * pre_up * sig_gate * (1.0 + pre_gate * (1.0 - sig_gate))).astype(jnp.bfloat16)
            up_b = (act_grad * pre_gate * sig_gate).astype(jnp.bfloat16)
            grads_gate.append(jnp.dot(slot_x.T, gate_b, preferred_element_type=jnp.float32).astype(jnp.bfloat16))
            grads_up.append(jnp.dot(slot_x.T, up_b, preferred_element_type=jnp.float32).astype(jnp.bfloat16))
            gate_split = gate_b.astype(jnp.float32).reshape(rows_max, N_TP, ff_local)
            up_split = up_b.astype(jnp.float32).reshape(rows_max, N_TP, ff_local)
            wg_split = local_gate[expert].astype(jnp.float32).reshape(D, N_TP, ff_local)
            wu_split = local_up[expert].astype(jnp.float32).reshape(D, N_TP, ff_local)
            blocks = blocks + jnp.einsum('rnf,dnf->nrd', gate_split, wg_split)
            blocks = blocks + jnp.einsum('rnf,dnf->nrd', up_split, wu_split)
        rounded = lax.optimization_barrier(blocks.astype(jnp.bfloat16)).astype(jnp.float32)
        dx_rows = jnp.sum(rounded, axis=0).astype(jnp.bfloat16)
        return (dx_rows, jnp.stack(gate_parts, axis=1), row_ids, is_valid,
                jnp.stack(grads_gate), jnp.stack(grads_up), jnp.stack(grads_down))

    dx_all, gate_all, rows_all, valid_all, gg_all, gu_all, gd_all = lax.map(
        one_group, jnp.arange(GROUPS, dtype=jnp.int32))
    flat_rows = rows_all.reshape(-1)
    flat_valid = valid_all.reshape(-1)[:, None]
    dx_flat = jnp.where(flat_valid, dx_all.reshape(-1, D).astype(jnp.float32), 0.0)
    tokens_grad = jnp.zeros((TOKENS, D), jnp.float32).at[flat_rows].add(dx_flat).astype(jnp.bfloat16)
    gate_flat = jnp.where(flat_valid, gate_all.reshape(-1, GROUP_EXPERTS), 0.0)
    dense_gate = jnp.zeros((TOKENS, GROUP_EXPERTS), jnp.float32).at[flat_rows].add(gate_flat)
    gate_grad = jnp.sum(chosen * dense_gate[:, None, :], axis=2)
    w_gate_grad = gg_all.reshape(EXPERTS, D, FF)
    w_up_grad = gu_all.reshape(EXPERTS, D, FF)
    w_down_grad = gd_all.reshape(EXPERTS, FF, D)
    return tokens_grad, gate_grad, w_gate_grad, w_up_grad, w_down_grad
```

```python
import jax
import jax.numpy as jnp
from jax import lax
from jax.sharding import Mesh, PartitionSpec as P

BF16, F32, F16 = jnp.bfloat16, jnp.float32, jnp.float16
TOP = 16384.0
LEAST = 1e-30


def swap(value, axis):
    return lax.all_to_all(value, axis, split_axis=0, concat_axis=0, tiled=True)


def on_device(tokens, cotangent, group_ids, within_ids, gate_weights, w_gate, w_up, w_down):
    eps = lax.axis_size("ep")
    xs, cs = lax.axis_size("x"), lax.axis_size("c")
    tps = xs * cs
    rows, width = tokens.shape
    experts, _, hidden = w_gate.shape
    cap = (3 * rows + 2 * eps - 1) // (2 * eps)
    slots = eps * cap
    share = width // tps

    group_of = group_ids[:, 0]
    in_group = (group_of[:, None] == jnp.arange(eps, dtype=jnp.int32)[None, :]).astype(BF16)
    at = jnp.arange(rows, dtype=jnp.int32)
    earlier = (at[:, None] > at[None, :]).astype(BF16)
    before = jnp.dot(earlier, in_group, preferred_element_type=F32)
    rank = jnp.sum(before * in_group.astype(F32), axis=1).astype(jnp.int32)
    target = group_of * cap + rank
    place = (jnp.arange(slots, dtype=jnp.int32)[:, None] == target[None, :]).astype(BF16)
    local = jnp.arange(experts, dtype=jnp.int32)
    chosen = (within_ids[:, :, None] == local[None, None, :]).astype(F32)
    combine = jnp.sum(chosen * gate_weights.astype(F32)[:, :, None], axis=1).astype(BF16)
    top_x = jnp.max(jnp.abs(tokens), axis=1, keepdims=True)
    top_dy = jnp.max(jnp.abs(cotangent), axis=1, keepdims=True)

    start = (lax.axis_index("x") * cs + lax.axis_index("c")) * share
    part_x = lax.dynamic_slice_in_dim(tokens, start, share, 1)
    part_dy = lax.dynamic_slice_in_dim(cotangent, start, share, 1)
    source = jnp.concatenate([part_x, part_dy, combine, top_x, top_dy], axis=1)
    sent = jnp.dot(place, source, preferred_element_type=F32).astype(BF16)
    got = swap(sent.reshape(eps, cap, source.shape[1]), "ep").reshape(slots, source.shape[1])
    comb = got[:, 2 * share : 2 * share + experts].astype(F32)
    top = jnp.maximum(got[:, 2 * share + experts :].astype(F32), LEAST)
    up = TOP / top
    down = top * (1.0 / TOP)
    scale = jnp.repeat(up, share, axis=1)
    thin = (got[:, : 2 * share].astype(F32) * scale).astype(F16)
    full = lax.all_gather(thin, ("x", "c"))

    def whole(part, back):
        value = (part.astype(F32) * back[None]).astype(BF16)
        return jnp.moveaxis(value, 0, 1).reshape(slots, width)

    slot_x = whole(full[:, :, :share], down[:, 0:1])
    slot_dy = whole(full[:, :, share:], down[:, 1:2])

    wide = experts * hidden
    w_in = jnp.concatenate([w_gate[e] for e in range(experts)] + [w_up[e] for e in range(experts)], axis=1)
    w_out = w_down.reshape(wide, width)
    pre = jnp.dot(slot_x, w_in, preferred_element_type=F32)
    grad = jnp.einsum("sd,fd->sf", slot_dy, w_out, preferred_element_type=F32)
    pre_gate, pre_up = pre[:, :wide], pre[:, wide:]
    weight = jnp.repeat(comb, hidden, axis=1)
    sig = jax.nn.sigmoid(pre_gate)
    silu = pre_gate * sig
    act = (silu * pre_up).astype(BF16).astype(F32)
    gate_part = jnp.sum((act * grad).reshape(slots, experts, hidden), axis=2)
    act_grad = weight * grad
    gate_b = (act_grad * pre_up * sig * (1.0 + pre_gate * (1.0 - sig))).astype(BF16)
    up_b = (act_grad * silu).astype(BF16)
    both = jnp.concatenate([gate_b, up_b], axis=1)
    w_blocks = w_in.reshape(tps, share, 2 * wide)
    dx = jnp.einsum("sf,kdf->ksd", both, w_blocks, preferred_element_type=F32).astype(BF16)

    lines = slots * experts // share
    spare = -lines % 16
    gate_rows = jnp.pad(gate_part.astype(BF16).reshape(lines, share), ((0, spare), (0, 0)))
    gate_rows = jnp.broadcast_to(gate_rows, (tps, lines + spare, share))
    blocks = jnp.concatenate([dx, gate_rows], axis=1)
    tall = blocks.shape[1]
    blocks = jnp.moveaxis(blocks.reshape(xs, cs, tall, share), 1, 0)
    pair = jnp.sum(swap(blocks, "c").astype(F32), axis=0).astype(BF16)
    total = jnp.sum(swap(pair, "x").astype(F32), axis=0)
    dx_share = total[:slots].astype(BF16)
    gate_sum = total[slots : slots + lines].reshape(slots, experts)
    gate_hi = gate_sum.astype(BF16)
    gate_lo = (gate_sum - gate_hi.astype(F32)).astype(BF16)

    home = jnp.concatenate([dx_share, gate_hi, gate_lo], axis=1)
    home = swap(home.reshape(eps, cap, home.shape[1]), "ep").reshape(slots, home.shape[1])
    own = jnp.einsum("st,sd->td", place, home, preferred_element_type=F32)
    tokens_grad = own[:, :share].astype(BF16)
    dense = own[:, share : share + experts] + own[:, share + experts :]
    gate_grad = jnp.sum(chosen * dense[:, None, :], axis=2)

    w_in_grad = jnp.einsum("sd,sf->df", slot_x, both, preferred_element_type=F32).astype(BF16)
    scaled_act = (act * weight).astype(BF16)
    w_down_grad = jnp.einsum("sf,sd->fd", scaled_act, slot_dy, preferred_element_type=F32).astype(BF16)
    pieces = [w_in_grad[:, i * hidden : (i + 1) * hidden] for i in range(2 * experts)]
    return (
        tokens_grad,
        gate_grad,
        jnp.stack(pieces[:experts]),
        jnp.stack(pieces[experts:]),
        w_down_grad.reshape(experts, hidden, width),
    )


def solution(mesh):
    eps, tps = mesh.shape["ep"], mesh.shape["tp"]
    fine = Mesh(mesh.devices.reshape(eps, tps // 2, 2), ("ep", "x", "c"))
    tp = ("x", "c")
    rows = P("ep", None)
    in_specs = (rows, rows, rows, rows, rows, P("ep", None, tp), P("ep", None, tp), P("ep", tp, None))
    out_specs = (P("ep", tp), rows, P("ep", None, tp), P("ep", None, tp), P("ep", tp, None))
    return jax.shard_map(on_device, mesh=fine, in_specs=in_specs, out_specs=out_specs, check_vma=False)
```

```python
import functools

import jax
import jax.numpy as jnp
from jax import lax
from jax.experimental import pallas as pl
from jax.experimental.pallas import tpu as pltpu
from jax.sharding import Mesh, PartitionSpec as P

BF16, F32, F16 = jnp.bfloat16, jnp.float32, jnp.float16
TILE = 8
VMEM = pl.BlockSpec(memory_space=pltpu.VMEM)
SMEM = pl.BlockSpec(memory_space=pltpu.SMEM)
ANY = pl.BlockSpec(memory_space=pl.ANY)


def swap(value, axis):
    return lax.all_to_all(value, axis, split_axis=0, concat_axis=0, tiled=True)


def dot(a, b, ca=1, cb=0):
    return lax.dot_general(a, b, (((ca,), (cb,)), ((), ())), preferred_element_type=F32)


def iota(shape, dim):
    return lax.broadcasted_iota(jnp.int32, shape, dim)


def call(body, outs, *args, flops=10**8, smem=0, scratch=(), held=(), room=20, **static):
    size = sum(a.size * a.dtype.itemsize for a in args[smem:]) + sum(o.size * o.dtype.itemsize for o in outs)
    return pl.pallas_call(
        functools.partial(body, **static) if static else body,
        out_shape=outs,
        in_specs=[SMEM if i < smem else ANY if i in held else VMEM for i in range(len(args))],
        out_specs=[VMEM] * len(outs),
        scratch_shapes=list(scratch),
        compiler_params=pltpu.CompilerParams(vmem_limit_bytes=room * 2**20),
        cost_estimate=pl.CostEstimate(flops=flops, bytes_accessed=size, transcendentals=0),
        name=body.__name__,
    )(*args)


def shape(*dims, dtype=BF16):
    return jax.ShapeDtypeStruct(dims, dtype)


def power(top):
    up, down = jnp.ones_like(top), jnp.ones_like(top)
    for k in (64, 32, 16, 8, 4, 2, 1):
        small = top < 2.0 ** (15 - k)
        step = jnp.where(small, 2.0**k, 1.0)
        top, up, down = top * step, up * step, down * jnp.where(small, 2.0**-k, 1.0)
    return up, down


def route(
    tp_ref, group_hbm, within_hbm, weight_hbm, x_hbm, dy_hbm, sent_ref, target_ref,
    group_ref, within_ref, weight_ref, x_ref, dy_ref, sems, *, eps, cap, share,
):
    pairs = (
        (group_hbm, group_ref), (within_hbm, within_ref), (weight_hbm, weight_ref), (x_hbm, x_ref), (dy_hbm, dy_ref)
    )
    copies = [pltpu.make_async_copy(hbm, ref, sems.at[i]) for i, (hbm, ref) in enumerate(pairs)]
    for copy in copies:
        copy.start()
    rows = x_ref.shape[0]
    for copy in copies[:3]:
        copy.wait()
    group = group_ref[...]
    member = iota((eps, rows), 0) == group
    earlier = (iota((rows, rows), 0) < iota((rows, rows), 1)).astype(BF16)
    before = dot(member.astype(BF16), earlier)
    rank = jnp.sum(jnp.where(member, before, 0.0), axis=0, keepdims=True).astype(jnp.int32)
    target = group * TILE + rank
    target_ref[...] = target
    row = iota((eps * TILE, rows), 0)
    place = (row == target).astype(BF16)
    beside = (row == target + cap).astype(BF16)
    within, weight = within_ref[...], weight_ref[...].astype(F32)
    expert = iota((share, rows), 0)
    combine = jnp.zeros((share, rows), F32)
    for k in range(within.shape[0]):
        combine = combine + jnp.where((expert == within[k : k + 1]) & (expert < 2), weight[k : k + 1], 0.0)
    sides = dot(beside, combine.astype(BF16), 1, 1)
    at = pl.multiple_of(tp_ref[0] * share, share)
    lane = iota((rows, share), 1)
    for copy in copies[3:]:
        copy.wait()
    parts, side = [], 0.0
    for i, ref in enumerate((x_ref, dy_ref)):
        top = jnp.max(jnp.abs(ref[...]), axis=1, keepdims=True).astype(F32)
        up, down = power(jnp.maximum(top, 2.0**-100))
        parts.append((ref[:, pl.ds(at, share)].astype(F32) * up).astype(BF16))
        side = side + jnp.where(lane == 2 + i, down, 0.0)
    sides = sides + dot(beside, side.astype(BF16))
    sent_ref[:, :share] = (dot(place, parts[0]) + sides).astype(BF16)
    sent_ref[:, share:] = dot(place, parts[1]).astype(BF16)


def split(value):
    hi = value.astype(BF16).astype(F32)
    return hi, value - hi


def four(first, second):
    a, b = split(first), split(second)
    return [a[0], b[0], a[1], b[1]]


def experts(
    c_ref, full_ref, got_ref, gate_ref, up_ref, down_ref, gate2_ref, up2_ref, down2_ref,
    out_ref, thin_ref, x_ref, dy_ref, *, cap,
):
    tps, slots, two = full_ref.shape
    share = two // 2
    wide = gate_ref.shape[0]
    for k in range(tps):
        x_ref[:, k * share : k * share + share] = full_ref[k, :, :share]
        dy_ref[:, k * share : k * share + share] = full_ref[k, :, share:]
    slot, row = iota((slots, got_ref.shape[0]), 0), iota((slots, got_ref.shape[0]), 1)
    pick = (row == slot // cap * TILE + cap + slot % cap).astype(BF16)
    side = dot(pick, got_ref[:, :share])
    back_x, back_dy = side[:, 2:3], side[:, 3:4]
    lane = iota((slots, 2 * wide), 1)
    weight = jnp.where(lane % wide < wide // 2, side[:, 0:1], side[:, 1:2])
    gates = jnp.concatenate([gate_ref[...], gate2_ref[...]], axis=0)
    ups = jnp.concatenate([up_ref[...], up2_ref[...]], axis=0)
    downs = jnp.concatenate([down_ref[...], down2_ref[...]], axis=0)
    pre_gate = dot(x_ref[...], gates, 1, 1) * back_x
    pre_up = dot(x_ref[...], ups, 1, 1) * back_x
    grad = dot(dy_ref[...], downs, 1, 1) * back_dy
    sig = jax.nn.sigmoid(pre_gate)
    silu = pre_gate * sig
    act = (silu * pre_up).astype(BF16).astype(F32)
    thin_ref[:, 2 * wide :] = (act * weight * back_dy)[:, :wide].astype(BF16)
    hi, lo = split(act * grad)
    ones = (iota((16, 2 * wide), 0) == iota((16, 2 * wide), 1) % wide // (wide // 2)).astype(BF16)
    sums = dot(ones, hi.astype(BF16), 1, 1) + dot(ones, lo.astype(BF16), 1, 1)
    lines = jnp.concatenate(four(sums[0:1], sums[1:2]), axis=0)
    lines = jnp.concatenate([lines[:, :share], lines[:, share:]], axis=0).astype(BF16)
    act_grad = weight * grad
    gate_b = (act_grad * pre_up * sig * (1.0 + pre_gate * (1.0 - sig))).astype(BF16)
    up_b = (act_grad * silu).astype(BF16)
    thin_ref[:, :wide] = (gate_b[:, :wide].astype(F32) * back_x).astype(BF16)
    thin_ref[:, wide : 2 * wide] = (up_b[:, :wide].astype(F32) * back_x).astype(BF16)
    for x in range(0, tps // 2, 2):
        at = [pl.ds(pl.multiple_of((2 * (x + i) + c_ref[0]) * share, share), share) for i in range(2)]
        dx = 0.0
        for value, refs in ((gate_b, (gate_ref, gate2_ref)), (up_b, (up_ref, up2_ref))):
            block = [jnp.concatenate([ref[:, a] for a in at], axis=1) for ref in refs]
            dx = dx + dot(value, jnp.concatenate(block, axis=0))
        for i in range(2):
            out_ref[x + i, :slots, :] = dx[:, i * share : i * share + share].astype(BF16)
            out_ref[x + i, slots:, :] = lines


def gather_up(blocks_ref, out_ref, *, cap):
    xs, tall, share = blocks_ref.shape
    slots = tall - 8
    total = blocks_ref[0].astype(F32)
    for x in range(1, xs):
        total = total + blocks_ref[x].astype(F32)
    dx = total[:slots].astype(BF16)
    lines = jnp.concatenate([total[slots : slots + 4], total[slots + 4 :]], axis=1)
    lines = four(lines[0:1] + lines[2:3], lines[1:2] + lines[3:4])
    lines = jnp.concatenate(lines + [jnp.zeros((share - 4, slots), F32)], axis=0).astype(BF16)
    row, slot = iota((out_ref.shape[0], slots), 0), iota((out_ref.shape[0], slots), 1)
    at = slot // cap * TILE + slot % cap
    out = dot((row == at).astype(BF16), dx) + dot((row == at + cap).astype(BF16), lines, 1, 1)
    out_ref[...] = out.astype(BF16)


def settle(target_ref, within_ref, home_ref, out_ref, gate_ref, *, cap):
    rows = out_ref.shape[0]
    row = iota((home_ref.shape[0], rows), 0)
    target = target_ref[...]
    home = home_ref[...]
    out_ref[...] = dot((row == target).astype(BF16), home, 0, 0).astype(BF16)
    dense = dot(home, (row == target + cap).astype(BF16), 0, 0)
    first = dense[0:1] + dense[2:3]
    second = dense[1:2] + dense[3:4]
    gate_ref[...] = jnp.where(within_ref[...] == 0, first, second)


def weights(full_ref, thin_ref, gate_ref, up_ref, down_ref):
    tps, slots, two = full_ref.shape
    share = two // 2
    wide = gate_ref.shape[0]
    for k in range(0, tps, 2):
        cols = slice(k * share, (k + 2) * share)
        x = jnp.concatenate([full_ref[k, :, :share], full_ref[k + 1, :, :share]], axis=1)
        dy = jnp.concatenate([full_ref[k, :, share:], full_ref[k + 1, :, share:]], axis=1)
        both = dot(thin_ref[:, : 2 * wide], x, 0, 0).astype(BF16)
        gate_ref[:, cols] = both[:wide]
        up_ref[:, cols] = both[wide:]
        down_ref[:, cols] = dot(thin_ref[:, 2 * wide :], dy, 0, 0).astype(BF16)


def on_device(tokens, cotangent, group_ids, within_ids, gate_weights, w_gate, w_up, w_down):
    eps = lax.axis_size("ep")
    xs, cs = lax.axis_size("x"), lax.axis_size("c")
    tps = xs * cs
    rows, width = tokens.shape
    count, _, hidden = w_gate.shape
    wide = count * hidden
    cap = (3 * rows + 2 * eps - 1) // (2 * eps)
    slots = eps * cap
    share = width // tps
    c = lax.axis_index("c").astype(jnp.int32)
    tp1 = (lax.axis_index("x").astype(jnp.int32) * cs + c).reshape(1)
    mine = (
        jnp.swapaxes(w_gate, 1, 2).reshape(wide, width),
        jnp.swapaxes(w_up, 1, 2).reshape(wide, width),
        w_down.reshape(wide, width),
    )
    within_t = within_ids.T

    sent, target = call(
        route,
        [shape(eps * TILE, 2 * share), shape(1, rows, dtype=jnp.int32)],
        tp1, group_ids.T, within_t, gate_weights.T, tokens, cotangent,
        smem=1, held=(1, 2, 3, 4, 5), room=58, eps=eps, cap=cap, share=share,
        scratch=[
            pltpu.VMEM((1, rows), jnp.int32), pltpu.VMEM((2, rows), jnp.int32), pltpu.VMEM((2, rows), BF16),
            pltpu.VMEM((rows, width), BF16), pltpu.VMEM((rows, width), BF16), pltpu.SemaphoreType.DMA((5,)),
        ],
    )
    got = swap(sent.reshape(eps, TILE, 2 * share), "ep")
    theirs = [lax.ppermute(w, "c", [(0, 1), (1, 0)]) for w in mine]
    thin = got[:, :cap, :].reshape(slots, 2 * share).astype(F16)
    full = lax.all_gather(thin, ("x", "c")).astype(BF16)

    blocks, thin_b = call(
        experts,
        [shape(xs, slots + 8, share), shape(slots, 3 * wide)],
        c.reshape(1), full, got.reshape(eps * TILE, 2 * share), *mine, *theirs,
        smem=1, flops=10**9, scratch=[pltpu.VMEM((slots, width), BF16)] * 2, cap=cap,
    )
    blocks = swap(blocks, "x")
    (home,) = call(gather_up, [shape(eps * TILE, share)], blocks, cap=cap)
    thin_b, home = lax.optimization_barrier((thin_b, home))
    home = swap(home.reshape(eps, TILE, share), "ep").reshape(eps * TILE, share)
    tokens_grad, gate_grad = call(
        settle, [shape(rows, share), shape(2, rows, dtype=F32)], target, within_t, home, cap=cap
    )
    gate_g, up_g, down_g = call(weights, [shape(wide, width)] * 3, full, thin_b, flops=10**9)
    return (
        tokens_grad,
        gate_grad.T,
        jnp.swapaxes(gate_g.reshape(count, hidden, width), 1, 2),
        jnp.swapaxes(up_g.reshape(count, hidden, width), 1, 2),
        down_g.reshape(count, hidden, width),
    )


def solution(mesh):
    eps, tps = mesh.shape["ep"], mesh.shape["tp"]
    fine = Mesh(mesh.devices.reshape(eps, tps // 2, 2), ("ep", "x", "c"))
    tp = ("x", "c")
    rows = P("ep", None)
    in_specs = (rows, rows, rows, rows, rows, P("ep", None, tp), P("ep", None, tp), P("ep", tp, None))
    out_specs = (P("ep", tp), rows, P("ep", None, tp), P("ep", None, tp), P("ep", tp, None))
    return jax.shard_map(on_device, mesh=fine, in_specs=in_specs, out_specs=out_specs, check_vma=False)
```

```python
import functools

import jax
import jax.numpy as jnp
from jax import lax
from jax.experimental import pallas as pl
from jax.experimental.pallas import tpu as pltpu
from jax.sharding import Mesh, PartitionSpec as P

BF16, F32, F16 = jnp.bfloat16, jnp.float32, jnp.float16
TILE = 8
VMEM = pl.BlockSpec(memory_space=pltpu.VMEM)
SMEM = pl.BlockSpec(memory_space=pltpu.SMEM)
ANY = pl.BlockSpec(memory_space=pl.ANY)


def swap(value, axis):
    return lax.all_to_all(value, axis, split_axis=0, concat_axis=0, tiled=True)


def dot(a, b, ca=1, cb=0):
    return lax.dot_general(a, b, (((ca,), (cb,)), ((), ())), preferred_element_type=F32)


def iota(shape, dim):
    return lax.broadcasted_iota(jnp.int32, shape, dim)


def call(body, outs, *args, flops=10**8, smem=0, scratch=(), held=(), room=20, **static):
    size = sum(a.size * a.dtype.itemsize for a in args[smem:]) + sum(o.size * o.dtype.itemsize for o in outs)
    return pl.pallas_call(
        functools.partial(body, **static) if static else body,
        out_shape=outs,
        in_specs=[SMEM if i < smem else ANY if i in held else VMEM for i in range(len(args))],
        out_specs=[VMEM] * len(outs),
        scratch_shapes=list(scratch),
        compiler_params=pltpu.CompilerParams(vmem_limit_bytes=room * 2**20),
        cost_estimate=pl.CostEstimate(flops=flops, bytes_accessed=size, transcendentals=0),
        name=body.__name__,
    )(*args)


def shape(*dims, dtype=BF16):
    return jax.ShapeDtypeStruct(dims, dtype)


def power(top):
    up, down = jnp.ones_like(top), jnp.ones_like(top)
    for k in (64, 32, 16, 8, 4, 2, 1):
        small = top < 2.0 ** (15 - k)
        step = jnp.where(small, 2.0**k, 1.0)
        top, up, down = top * step, up * step, down * jnp.where(small, 2.0**-k, 1.0)
    return up, down


def route(
    tp_ref, group_hbm, within_hbm, weight_hbm, x_hbm, dy_hbm, sent_ref, target_ref,
    group_ref, within_ref, weight_ref, x_ref, dy_ref, sems, *, eps, cap, share,
):
    pairs = (
        (group_hbm, group_ref), (within_hbm, within_ref), (weight_hbm, weight_ref), (x_hbm, x_ref), (dy_hbm, dy_ref)
    )
    copies = [pltpu.make_async_copy(hbm, ref, sems.at[i]) for i, (hbm, ref) in enumerate(pairs)]
    for copy in copies:
        copy.start()
    rows = x_ref.shape[0]
    for copy in copies[:3]:
        copy.wait()
    group = group_ref[...]
    member = iota((eps, rows), 0) == group
    earlier = (iota((rows, rows), 0) < iota((rows, rows), 1)).astype(BF16)
    before = dot(member.astype(BF16), earlier)
    rank = jnp.sum(jnp.where(member, before, 0.0), axis=0, keepdims=True).astype(jnp.int32)
    target = group * TILE + rank
    target_ref[...] = target
    row = iota((eps * TILE, rows), 0)
    place = (row == target).astype(BF16)
    beside = (row == target + cap).astype(BF16)
    within, weight = within_ref[...], weight_ref[...].astype(F32)
    expert = iota((share, rows), 0)
    combine = jnp.zeros((share, rows), F32)
    for k in range(within.shape[0]):
        combine = combine + jnp.where((expert == within[k : k + 1]) & (expert < 2), weight[k : k + 1], 0.0)
    sides = dot(beside, combine.astype(BF16), 1, 1)
    at = pl.multiple_of(tp_ref[0] * share, share)
    lane = iota((rows, share), 1)
    for copy in copies[3:]:
        copy.wait()
    parts, side = [], 0.0
    for i, ref in enumerate((x_ref, dy_ref)):
        top = jnp.max(jnp.abs(ref[...]), axis=1, keepdims=True).astype(F32)
        up, down = power(jnp.maximum(top, 2.0**-100))
        parts.append((ref[:, pl.ds(at, share)].astype(F32) * up).astype(BF16))
        side = side + jnp.where(lane == 2 + i, down, 0.0)
    sides = sides + dot(beside, side.astype(BF16))
    sent_ref[:, :share] = (dot(place, parts[0]) + sides).astype(BF16)
    sent_ref[:, share:] = dot(place, parts[1]).astype(BF16)


def split(value):
    hi = value.astype(BF16).astype(F32)
    return hi, value - hi


def four(first, second):
    a, b = split(first), split(second)
    return [a[0], b[0], a[1], b[1]]


def experts(
    c_ref, full_ref, got_ref, mine_hbm, theirs_hbm, out_ref, thin_ref, x_ref, dy_ref, in_ref, down_ref, sems, *, cap
):
    tps, slots, two = full_ref.shape
    share = two // 2
    wide = down_ref.shape[0] // 2
    piece = wide // 2
    copies = []
    for i, hbm in enumerate((mine_hbm, theirs_hbm)):
        for j in range(6):
            ref, at = (in_ref, 2 * wide * i + piece * j) if j < 4 else (down_ref, wide * i + piece * (j - 4))
            copies.append(
                pltpu.make_async_copy(hbm.at[pl.ds(piece * j, piece)], ref.at[pl.ds(at, piece)], sems.at[i, j])
            )
            copies[-1].start()
    for k in range(tps):
        x_ref[:, k * share : k * share + share] = full_ref[k, :, :share]
        dy_ref[:, k * share : k * share + share] = full_ref[k, :, share:]
    slot, row = iota((slots, got_ref.shape[0]), 0), iota((slots, got_ref.shape[0]), 1)
    pick = (row == slot // cap * TILE + cap + slot % cap).astype(BF16)
    side = dot(pick, got_ref[:, :share])
    for copy in copies:
        copy.wait()
    back_x, back_dy = side[:, 2:3], side[:, 3:4]
    lane = iota((slots, 2 * wide), 1)
    weight = jnp.where(lane % wide < wide // 2, side[:, 0:1], side[:, 1:2])
    pre = dot(x_ref[...], in_ref[...], 1, 1) * back_x
    grad = dot(dy_ref[...], down_ref[...], 1, 1) * back_dy
    pre_gate = jnp.concatenate([pre[:, :wide], pre[:, 2 * wide : 3 * wide]], axis=1)
    pre_up = jnp.concatenate([pre[:, wide : 2 * wide], pre[:, 3 * wide :]], axis=1)
    sig = jax.nn.sigmoid(pre_gate)
    silu = pre_gate * sig
    act = (silu * pre_up).astype(BF16).astype(F32)
    act_grad = weight * grad
    gate_b = (act_grad * pre_up * sig * (1.0 + pre_gate * (1.0 - sig))).astype(BF16)
    up_b = (act_grad * silu).astype(BF16)
    both = jnp.concatenate([gate_b[:, :wide], up_b[:, :wide], gate_b[:, wide:], up_b[:, wide:]], axis=1)
    thin_ref[:, : 2 * wide] = (both[:, : 2 * wide].astype(F32) * back_x).astype(BF16)
    thin_ref[:, 2 * wide :] = (act * weight * back_dy)[:, :wide].astype(BF16)
    hi, lo = split(act * grad)
    ones = (iota((16, 2 * wide), 0) == iota((16, 2 * wide), 1) % wide // (wide // 2)).astype(BF16)
    sums = dot(ones, hi.astype(BF16), 1, 1) + dot(ones, lo.astype(BF16), 1, 1)
    lines = jnp.concatenate(four(sums[0:1], sums[1:2]), axis=0)
    lines = jnp.concatenate([lines[:, :share], lines[:, share:]], axis=0).astype(BF16)
    for x in range(0, tps // 2, 2):
        at = [pl.ds(pl.multiple_of((2 * (x + i) + c_ref[0]) * share, share), share) for i in range(2)]
        dx = dot(both, jnp.concatenate([in_ref[:, a] for a in at], axis=1))
        for i in range(2):
            out_ref[x + i, :slots, :] = dx[:, i * share : i * share + share].astype(BF16)
            out_ref[x + i, slots:, :] = lines


def gather_up(blocks_ref, out_ref, *, cap):
    xs, tall, share = blocks_ref.shape
    slots = tall - 8
    total = blocks_ref[0].astype(F32)
    for x in range(1, xs):
        total = total + blocks_ref[x].astype(F32)
    dx = total[:slots].astype(BF16)
    lines = jnp.concatenate([total[slots : slots + 4], total[slots + 4 :]], axis=1)
    lines = four(lines[0:1] + lines[2:3], lines[1:2] + lines[3:4])
    lines = jnp.concatenate(lines + [jnp.zeros((share - 4, slots), F32)], axis=0).astype(BF16)
    row, slot = iota((out_ref.shape[0], slots), 0), iota((out_ref.shape[0], slots), 1)
    at = slot // cap * TILE + slot % cap
    out = dot((row == at).astype(BF16), dx) + dot((row == at + cap).astype(BF16), lines, 1, 1)
    out_ref[...] = out.astype(BF16)


def settle(target_ref, within_ref, home_ref, out_ref, gate_ref, *, cap):
    rows = out_ref.shape[0]
    row = iota((home_ref.shape[0], rows), 0)
    target = target_ref[...]
    home = home_ref[...]
    out_ref[...] = dot((row == target).astype(BF16), home, 0, 0).astype(BF16)
    dense = dot(home, (row == target + cap).astype(BF16), 0, 0)
    first = dense[0:1] + dense[2:3]
    second = dense[1:2] + dense[3:4]
    gate_ref[...] = jnp.where(within_ref[...] == 0, first, second)


def weights(full_ref, thin_ref, gate_ref, up_ref, down_ref):
    tps, slots, two = full_ref.shape
    share = two // 2
    wide = gate_ref.shape[0]
    for k in range(0, tps, 2):
        cols = slice(k * share, (k + 2) * share)
        x = jnp.concatenate([full_ref[k, :, :share], full_ref[k + 1, :, :share]], axis=1)
        dy = jnp.concatenate([full_ref[k, :, share:], full_ref[k + 1, :, share:]], axis=1)
        both = dot(thin_ref[:, : 2 * wide], x, 0, 0).astype(BF16)
        gate_ref[:, cols] = both[:wide]
        up_ref[:, cols] = both[wide:]
        down_ref[:, cols] = dot(thin_ref[:, 2 * wide :], dy, 0, 0).astype(BF16)


def on_device(tokens, cotangent, group_ids, within_ids, gate_weights, w_gate, w_up, w_down):
    eps = lax.axis_size("ep")
    xs, cs = lax.axis_size("x"), lax.axis_size("c")
    tps = xs * cs
    rows, width = tokens.shape
    count, _, hidden = w_gate.shape
    wide = count * hidden
    cap = (3 * rows + 2 * eps - 1) // (2 * eps)
    slots = eps * cap
    share = width // tps
    c = lax.axis_index("c").astype(jnp.int32)
    tp1 = (lax.axis_index("x").astype(jnp.int32) * cs + c).reshape(1)
    mine = jnp.concatenate([jnp.swapaxes(w_gate, 1, 2), jnp.swapaxes(w_up, 1, 2), w_down]).reshape(3 * wide, width)
    within_t = within_ids.T

    sent, target = call(
        route,
        [shape(eps * TILE, 2 * share), shape(1, rows, dtype=jnp.int32)],
        tp1, group_ids.T, within_t, gate_weights.T, tokens, cotangent,
        smem=1, held=(1, 2, 3, 4, 5), room=58, eps=eps, cap=cap, share=share,
        scratch=[
            pltpu.VMEM((1, rows), jnp.int32), pltpu.VMEM((2, rows), jnp.int32), pltpu.VMEM((2, rows), BF16),
            pltpu.VMEM((rows, width), BF16), pltpu.VMEM((rows, width), BF16), pltpu.SemaphoreType.DMA((5,)),
        ],
    )
    got = swap(sent.reshape(eps, TILE, 2 * share), "ep")
    theirs = lax.ppermute(mine, "c", [(0, 1), (1, 0)])
    thin = got[:, :cap, :].reshape(slots, 2 * share).astype(F16)
    full = lax.all_gather(thin, ("x", "c")).astype(BF16)

    blocks, thin_b = call(
        experts,
        [shape(xs, slots + 8, share), shape(slots, 3 * wide)],
        c.reshape(1), full, got.reshape(eps * TILE, 2 * share), mine, theirs,
        smem=1, held=(3, 4), flops=10**9, cap=cap,
        scratch=[pltpu.VMEM((slots, width), BF16)] * 2
        + [pltpu.VMEM((4 * wide, width), BF16), pltpu.VMEM((2 * wide, width), BF16), pltpu.SemaphoreType.DMA((2, 6))],
    )
    blocks = swap(blocks, "x")
    (home,) = call(gather_up, [shape(eps * TILE, share)], blocks, cap=cap)
    thin_b, home = lax.optimization_barrier((thin_b, home))
    home = swap(home.reshape(eps, TILE, share), "ep").reshape(eps * TILE, share)
    tokens_grad, gate_grad = call(
        settle, [shape(rows, share), shape(2, rows, dtype=F32)], target, within_t, home, cap=cap
    )
    gate_g, up_g, down_g = call(weights, [shape(wide, width)] * 3, full, thin_b, flops=10**9)
    return (
        tokens_grad,
        gate_grad.T,
        jnp.swapaxes(gate_g.reshape(count, hidden, width), 1, 2),
        jnp.swapaxes(up_g.reshape(count, hidden, width), 1, 2),
        down_g.reshape(count, hidden, width),
    )


def solution(mesh):
    eps, tps = mesh.shape["ep"], mesh.shape["tp"]
    fine = Mesh(mesh.devices.reshape(eps, tps // 2, 2), ("ep", "x", "c"))
    tp = ("x", "c")
    rows = P("ep", None)
    in_specs = (rows, rows, rows, rows, rows, P("ep", None, tp), P("ep", None, tp), P("ep", tp, None))
    out_specs = (P("ep", tp), rows, P("ep", None, tp), P("ep", None, tp), P("ep", tp, None))
    return jax.shard_map(on_device, mesh=fine, in_specs=in_specs, out_specs=out_specs, check_vma=False)
```

```python
import functools

import jax
import jax.numpy as jnp
from jax import lax
from jax.experimental import pallas as pl
from jax.experimental.pallas import tpu as pltpu
from jax.sharding import Mesh, PartitionSpec as P

BF16, F32, F16 = jnp.bfloat16, jnp.float32, jnp.float16
TILE = 8
VMEM = pl.BlockSpec(memory_space=pltpu.VMEM)
SMEM = pl.BlockSpec(memory_space=pltpu.SMEM)
ANY = pl.BlockSpec(memory_space=pl.ANY)


def swap(value, axis):
    return lax.all_to_all(value, axis, split_axis=0, concat_axis=0, tiled=True)


def dot(a, b, ca=1, cb=0):
    return lax.dot_general(a, b, (((ca,), (cb,)), ((), ())), preferred_element_type=F32)


def iota(shape, dim):
    return lax.broadcasted_iota(jnp.int32, shape, dim)


def call(body, outs, *args, flops=10**8, smem=0, scratch=(), held=(), room=20, **static):
    size = sum(a.size * a.dtype.itemsize for a in args[smem:]) + sum(o.size * o.dtype.itemsize for o in outs)
    return pl.pallas_call(
        functools.partial(body, **static) if static else body,
        out_shape=outs,
        in_specs=[SMEM if i < smem else ANY if i in held else VMEM for i in range(len(args))],
        out_specs=[VMEM] * len(outs),
        scratch_shapes=list(scratch),
        compiler_params=pltpu.CompilerParams(vmem_limit_bytes=room * 2**20),
        cost_estimate=pl.CostEstimate(flops=flops, bytes_accessed=size, transcendentals=0),
        name=body.__name__,
    )(*args)


def shape(*dims, dtype=BF16):
    return jax.ShapeDtypeStruct(dims, dtype)


def power(top):
    up, down = jnp.ones_like(top), jnp.ones_like(top)
    for k in (64, 32, 16, 8, 4, 2, 1):
        small = top < 2.0 ** (15 - k)
        step = jnp.where(small, 2.0**k, 1.0)
        top, up, down = top * step, up * step, down * jnp.where(small, 2.0**-k, 1.0)
    return up, down


def route(
    tp_ref, group_hbm, within_hbm, weight_hbm, x_hbm, dy_hbm, sent_ref, target_ref,
    group_ref, within_ref, weight_ref, x_ref, dy_ref, sems, *, eps, cap, share,
):
    pairs = (
        (group_hbm, group_ref), (within_hbm, within_ref), (weight_hbm, weight_ref), (x_hbm, x_ref), (dy_hbm, dy_ref)
    )
    copies = [pltpu.make_async_copy(hbm, ref, sems.at[i]) for i, (hbm, ref) in enumerate(pairs)]
    for copy in copies:
        copy.start()
    rows = x_ref.shape[0]
    for copy in copies[:3]:
        copy.wait()
    group = group_ref[...]
    member = iota((eps, rows), 0) == group
    earlier = (iota((rows, rows), 0) < iota((rows, rows), 1)).astype(BF16)
    before = dot(member.astype(BF16), earlier)
    rank = jnp.sum(jnp.where(member, before, 0.0), axis=0, keepdims=True).astype(jnp.int32)
    target = group * TILE + rank
    target_ref[...] = target
    row = iota((eps * TILE, rows), 0)
    place = (row == target).astype(BF16)
    beside = (row == target + cap).astype(BF16)
    within, weight = within_ref[...], weight_ref[...].astype(F32)
    expert = iota((share, rows), 0)
    combine = jnp.zeros((share, rows), F32)
    for k in range(within.shape[0]):
        combine = combine + jnp.where((expert == within[k : k + 1]) & (expert < 2), weight[k : k + 1], 0.0)
    sides = dot(beside, combine.astype(BF16), 1, 1)
    at = pl.multiple_of(tp_ref[0] * share, share)
    lane = iota((rows, share), 1)
    for copy in copies[3:]:
        copy.wait()
    parts, side = [], 0.0
    for i, ref in enumerate((x_ref, dy_ref)):
        top = jnp.max(jnp.abs(ref[...]), axis=1, keepdims=True).astype(F32)
        up, down = power(jnp.maximum(top, 2.0**-100))
        parts.append((ref[:, pl.ds(at, share)].astype(F32) * up).astype(BF16))
        side = side + jnp.where(lane == 2 + i, down, 0.0)
    sides = sides + dot(beside, side.astype(BF16))
    sent_ref[:, :share] = (dot(place, parts[0]) + sides).astype(BF16)
    sent_ref[:, share:] = dot(place, parts[1]).astype(BF16)


def split(value):
    hi = value.astype(BF16).astype(F32)
    return hi, value - hi


def four(first, second):
    a, b = split(first), split(second)
    return [a[0], b[0], a[1], b[1]]


def experts(
    c_ref, full_ref, got_ref, mine_hbm, theirs_hbm, out_ref, thin_ref, x_ref, dy_ref, in_ref, down_ref, sems, *, cap
):
    tps, slots, two = full_ref.shape
    share = two // 2
    wide = down_ref.shape[0] // 2
    piece = wide // 2
    copies = []
    for i, hbm in enumerate((mine_hbm, theirs_hbm)):
        for j in range(6):
            ref, at = (in_ref, 2 * wide * i + piece * j) if j < 4 else (down_ref, wide * i + piece * (j - 4))
            copies.append(
                pltpu.make_async_copy(hbm.at[pl.ds(piece * j, piece)], ref.at[pl.ds(at, piece)], sems.at[i, j])
            )
    for i in (0, 1, 2, 3, 6, 7, 8, 9, 4, 5, 10, 11):
        copies[i].start()
    for k in range(tps):
        x_ref[:, k * share : k * share + share] = full_ref[k, :, :share]
        dy_ref[:, k * share : k * share + share] = full_ref[k, :, share:]
    slot = iota((slots, 1), 0)
    pick = (iota((slots, got_ref.shape[0]), 1) == slot // cap * TILE + cap + slot % cap).astype(BF16)
    side = dot(pick, got_ref[:, :share])
    for i in (0, 1, 2, 3, 6, 7, 8, 9):
        copies[i].wait()
    back_x, back_dy = side[:, 2:3], side[:, 3:4]
    weight = jnp.where(iota((1, 2 * wide), 1) % wide < wide // 2, side[:, 0:1], side[:, 1:2])
    pre = dot(x_ref[...], in_ref[...], 1, 1) * back_x
    for i in (4, 5, 10, 11):
        copies[i].wait()
    grad = dot(dy_ref[...], down_ref[...], 1, 1) * back_dy
    pre_gate = jnp.concatenate([pre[:, :wide], pre[:, 2 * wide : 3 * wide]], axis=1)
    pre_up = jnp.concatenate([pre[:, wide : 2 * wide], pre[:, 3 * wide :]], axis=1)
    sig = jax.nn.sigmoid(pre_gate)
    silu = pre_gate * sig
    act = (silu * pre_up).astype(BF16).astype(F32)
    act_grad = weight * grad
    gate_b = (act_grad * pre_up * sig * (1.0 + pre_gate * (1.0 - sig))).astype(BF16)
    up_b = (act_grad * silu).astype(BF16)
    both = jnp.concatenate([gate_b[:, :wide], up_b[:, :wide], gate_b[:, wide:], up_b[:, wide:]], axis=1)
    thin_ref[:, : 2 * wide] = (both[:, : 2 * wide].astype(F32) * back_x).astype(BF16)
    thin_ref[:, 2 * wide :] = (act * weight * back_dy)[:, :wide].astype(BF16)
    hi, lo = split(act * grad)
    ones = (iota((16, 2 * wide), 0) == iota((16, 2 * wide), 1) % wide // (wide // 2)).astype(BF16)
    sums = dot(ones, hi.astype(BF16), 1, 1) + dot(ones, lo.astype(BF16), 1, 1)
    lines = jnp.concatenate(four(sums[0:1], sums[1:2]), axis=0)
    lines = jnp.concatenate([lines[:, :share], lines[:, share:]], axis=0).astype(BF16)
    for x in range(0, tps // 2, 2):
        at = [pl.ds(pl.multiple_of((2 * (x + i) + c_ref[0]) * share, share), share) for i in range(2)]
        dx = dot(both, jnp.concatenate([in_ref[:, a] for a in at], axis=1))
        for i in range(2):
            out_ref[x + i, :slots, :] = dx[:, i * share : i * share + share].astype(BF16)
            out_ref[x + i, slots:, :] = lines


def gather_up(blocks_ref, out_ref, *, cap):
    xs, tall, share = blocks_ref.shape
    slots = tall - 8
    total = blocks_ref[0].astype(F32)
    for x in range(1, xs):
        total = total + blocks_ref[x].astype(F32)
    dx = total[:slots].astype(BF16)
    lines = jnp.concatenate([total[slots : slots + 4], total[slots + 4 :]], axis=1)
    lines = four(lines[0:1] + lines[2:3], lines[1:2] + lines[3:4])
    lines = jnp.concatenate(lines + [jnp.zeros((share - 4, slots), F32)], axis=0).astype(BF16)
    row, slot = iota((out_ref.shape[0], slots), 0), iota((1, slots), 1)
    at = slot // cap * TILE + slot % cap
    out = dot((row == at).astype(BF16), dx) + dot((row == at + cap).astype(BF16), lines, 1, 1)
    out_ref[...] = out.astype(BF16)


def settle(target_ref, within_ref, home_ref, out_ref, gate_ref, *, cap):
    rows = out_ref.shape[0]
    row = iota((home_ref.shape[0], rows), 0)
    target = target_ref[...]
    home = home_ref[...]
    out_ref[...] = dot((row == target).astype(BF16), home, 0, 0).astype(BF16)
    dense = dot(home, (row == target + cap).astype(BF16), 0, 0)
    first = dense[0:1] + dense[2:3]
    second = dense[1:2] + dense[3:4]
    gate_ref[...] = jnp.where(within_ref[...] == 0, first, second)


def weights(full_ref, thin_ref, gate_ref, up_ref, down_ref):
    tps, slots, two = full_ref.shape
    share = two // 2
    wide = gate_ref.shape[0]
    for k in range(0, tps, 2):
        cols = slice(k * share, (k + 2) * share)
        x = jnp.concatenate([full_ref[k, :, :share], full_ref[k + 1, :, :share]], axis=1)
        dy = jnp.concatenate([full_ref[k, :, share:], full_ref[k + 1, :, share:]], axis=1)
        both = dot(thin_ref[:, : 2 * wide], x, 0, 0).astype(BF16)
        gate_ref[:, cols] = both[:wide]
        up_ref[:, cols] = both[wide:]
        down_ref[:, cols] = dot(thin_ref[:, 2 * wide :], dy, 0, 0).astype(BF16)


def on_device(tokens, cotangent, group_ids, within_ids, gate_weights, w_gate, w_up, w_down):
    eps = lax.axis_size("ep")
    xs, cs = lax.axis_size("x"), lax.axis_size("c")
    tps = xs * cs
    rows, width = tokens.shape
    count, _, hidden = w_gate.shape
    wide = count * hidden
    cap = (3 * rows + 2 * eps - 1) // (2 * eps)
    slots = eps * cap
    share = width // tps
    c = lax.axis_index("c").astype(jnp.int32)
    tp1 = (lax.axis_index("x").astype(jnp.int32) * cs + c).reshape(1)
    mine = jnp.concatenate([jnp.swapaxes(w_gate, 1, 2), jnp.swapaxes(w_up, 1, 2), w_down]).reshape(3 * wide, width)
    within_t = within_ids.T

    sent, target = call(
        route,
        [shape(eps * TILE, 2 * share), shape(1, rows, dtype=jnp.int32)],
        tp1, group_ids.T, within_t, gate_weights.T, tokens, cotangent,
        smem=1, held=(1, 2, 3, 4, 5), room=58, eps=eps, cap=cap, share=share,
        scratch=[
            pltpu.VMEM((1, rows), jnp.int32), pltpu.VMEM((2, rows), jnp.int32), pltpu.VMEM((2, rows), BF16),
            pltpu.VMEM((rows, width), BF16), pltpu.VMEM((rows, width), BF16), pltpu.SemaphoreType.DMA((5,)),
        ],
    )
    got = swap(sent.reshape(eps, TILE, 2 * share), "ep")
    theirs = lax.ppermute(mine, "c", [(0, 1), (1, 0)])
    thin = got[:, :cap, :].reshape(slots, 2 * share).astype(F16)
    full = lax.all_gather(thin, ("x", "c")).astype(BF16)

    blocks, thin_b = call(
        experts,
        [shape(xs, slots + 8, share), shape(slots, 3 * wide)],
        c.reshape(1), full, got.reshape(eps * TILE, 2 * share), mine, theirs,
        smem=1, held=(3, 4), flops=10**9, cap=cap,
        scratch=[pltpu.VMEM((slots, width), BF16)] * 2
        + [pltpu.VMEM((4 * wide, width), BF16), pltpu.VMEM((2 * wide, width), BF16), pltpu.SemaphoreType.DMA((2, 6))],
    )
    blocks = swap(blocks, "x")
    (home,) = call(gather_up, [shape(eps * TILE, share)], blocks, cap=cap)
    thin_b, home = lax.optimization_barrier((thin_b, home))
    home = swap(home.reshape(eps, TILE, share), "ep").reshape(eps * TILE, share)
    tokens_grad, gate_grad = call(
        settle, [shape(rows, share), shape(2, rows, dtype=F32)], target, within_t, home, cap=cap
    )
    gate_g, up_g, down_g = call(weights, [shape(wide, width)] * 3, full, thin_b, flops=10**9)
    return (
        tokens_grad,
        gate_grad.T,
        jnp.swapaxes(gate_g.reshape(count, hidden, width), 1, 2),
        jnp.swapaxes(up_g.reshape(count, hidden, width), 1, 2),
        down_g.reshape(count, hidden, width),
    )


def solution(mesh):
    eps, tps = mesh.shape["ep"], mesh.shape["tp"]
    fine = Mesh(mesh.devices.reshape(eps, tps // 2, 2), ("ep", "x", "c"))
    tp = ("x", "c")
    rows = P("ep", None)
    in_specs = (rows, rows, rows, rows, rows, P("ep", None, tp), P("ep", None, tp), P("ep", tp, None))
    out_specs = (P("ep", tp), rows, P("ep", None, tp), P("ep", None, tp), P("ep", tp, None))
    return jax.shard_map(on_device, mesh=fine, in_specs=in_specs, out_specs=out_specs, check_vma=False)
```

```python
import functools

import jax
import jax.numpy as jnp
from jax import lax
from jax.experimental import pallas as pl
from jax.experimental.pallas import tpu as pltpu
from jax.sharding import Mesh, PartitionSpec as P

BF16, F32, F16 = jnp.bfloat16, jnp.float32, jnp.float16
TILE = 8
VMEM = pl.BlockSpec(memory_space=pltpu.VMEM)
SMEM = pl.BlockSpec(memory_space=pltpu.SMEM)
ANY = pl.BlockSpec(memory_space=pl.ANY)


def swap(value, axis):
    return lax.all_to_all(value, axis, split_axis=0, concat_axis=0, tiled=True)


def dot(a, b, ca=1, cb=0):
    return lax.dot_general(a, b, (((ca,), (cb,)), ((), ())), preferred_element_type=F32)


def iota(shape, dim):
    return lax.broadcasted_iota(jnp.int32, shape, dim)


def call(body, outs, *args, flops=10**8, smem=0, scratch=(), held=(), room=20, **static):
    size = sum(a.size * a.dtype.itemsize for a in args[smem:]) + sum(o.size * o.dtype.itemsize for o in outs)
    return pl.pallas_call(
        functools.partial(body, **static) if static else body,
        out_shape=outs,
        in_specs=[SMEM if i < smem else ANY if i in held else VMEM for i in range(len(args))],
        out_specs=[VMEM] * len(outs),
        scratch_shapes=list(scratch),
        compiler_params=pltpu.CompilerParams(vmem_limit_bytes=room * 2**20),
        cost_estimate=pl.CostEstimate(flops=flops, bytes_accessed=size, transcendentals=0),
        name=body.__name__,
    )(*args)


def shape(*dims, dtype=BF16):
    return jax.ShapeDtypeStruct(dims, dtype)


def power(top):
    up, down = jnp.ones_like(top), jnp.ones_like(top)
    for k in (64, 32, 16, 8, 4, 2, 1):
        small = top < 2.0 ** (15 - k)
        step = jnp.where(small, 2.0**k, 1.0)
        top, up, down = top * step, up * step, down * jnp.where(small, 2.0**-k, 1.0)
    return up, down


def route(
    tp_ref, group_hbm, within_hbm, weight_hbm, x_hbm, dy_hbm, sent_ref, target_ref,
    group_ref, within_ref, weight_ref, x_ref, dy_ref, sems, *, eps, cap, share,
):
    pairs = (
        (group_hbm, group_ref), (within_hbm, within_ref), (weight_hbm, weight_ref), (x_hbm, x_ref), (dy_hbm, dy_ref)
    )
    copies = [pltpu.make_async_copy(hbm, ref, sems.at[i]) for i, (hbm, ref) in enumerate(pairs)]
    for copy in copies:
        copy.start()
    rows = x_ref.shape[0]
    for copy in copies[:3]:
        copy.wait()
    group = group_ref[...]
    member = iota((eps, rows), 0) == group
    earlier = (iota((rows, rows), 0) < iota((rows, rows), 1)).astype(BF16)
    before = dot(member.astype(BF16), earlier)
    rank = jnp.sum(jnp.where(member, before, 0.0), axis=0, keepdims=True).astype(jnp.int32)
    target = group * TILE + rank
    target_ref[...] = target
    row = iota((eps * TILE, rows), 0)
    place = (row == target).astype(BF16)
    beside = (row == target + cap).astype(BF16)
    within, weight = within_ref[...], weight_ref[...].astype(F32)
    expert = iota((share, rows), 0)
    combine = jnp.zeros((share, rows), F32)
    for k in range(within.shape[0]):
        combine = combine + jnp.where((expert == within[k : k + 1]) & (expert < 2), weight[k : k + 1], 0.0)
    sides = dot(beside, combine.astype(BF16), 1, 1)
    at = pl.multiple_of(tp_ref[0] * share, share)
    lane = iota((rows, share), 1)
    for copy in copies[3:]:
        copy.wait()
    tops = [jnp.max(jnp.abs(ref[...]), axis=1, keepdims=True).astype(F32) for ref in (x_ref, dy_ref)]
    up, down = power(jnp.maximum(jnp.where(lane == 2, tops[0], tops[1]), 2.0**-100))
    side = jnp.where((lane == 2) | (lane == 3), down, 0.0)
    parts = [
        (ref[:, pl.ds(at, share)].astype(F32) * up[:, 2 + i : 3 + i]).astype(BF16)
        for i, ref in enumerate((x_ref, dy_ref))
    ]
    sides = sides + dot(beside, side.astype(BF16))
    sent_ref[:, :share] = (dot(place, parts[0]) + sides).astype(BF16)
    sent_ref[:, share:] = dot(place, parts[1]).astype(BF16)


def split(value):
    hi = value.astype(BF16).astype(F32)
    return hi, value - hi


def four(first, second):
    a, b = split(first), split(second)
    return [a[0], b[0], a[1], b[1]]


def experts(
    c_ref, full_ref, got_ref, mine_hbm, theirs_hbm, out_ref, thin_ref, x_ref, dy_ref, in_ref, down_ref, sems, *, cap
):
    tps, slots, two = full_ref.shape
    share = two // 2
    wide = down_ref.shape[0] // 2
    piece = wide // 2
    copies = []
    for i, hbm in enumerate((mine_hbm, theirs_hbm)):
        for j in range(6):
            ref, at = (in_ref, 2 * wide * i + piece * j) if j < 4 else (down_ref, wide * i + piece * (j - 4))
            copies.append(
                pltpu.make_async_copy(hbm.at[pl.ds(piece * j, piece)], ref.at[pl.ds(at, piece)], sems.at[i, j])
            )
    for i in (0, 1, 2, 3, 6, 7, 8, 9, 4, 5, 10, 11):
        copies[i].start()
    for k in range(tps):
        x_ref[:, k * share : k * share + share] = full_ref[k, :, :share]
        dy_ref[:, k * share : k * share + share] = full_ref[k, :, share:]
    slot = iota((slots, 1), 0)
    pick = (iota((slots, got_ref.shape[0]), 1) == slot // cap * TILE + cap + slot % cap).astype(BF16)
    side = dot(pick, got_ref[:, :share])
    for i in (0, 1, 2, 3, 6, 7, 8, 9):
        copies[i].wait()
    back_x, back_dy = side[:, 2:3], side[:, 3:4]
    weight = jnp.where(iota((1, 2 * wide), 1) % wide < wide // 2, side[:, 0:1], side[:, 1:2])
    pre = dot(x_ref[...], in_ref[...], 1, 1) * back_x
    for i in (4, 5, 10, 11):
        copies[i].wait()
    grad = dot(dy_ref[...], down_ref[...], 1, 1) * back_dy
    pre_gate = jnp.concatenate([pre[:, :wide], pre[:, 2 * wide : 3 * wide]], axis=1)
    pre_up = jnp.concatenate([pre[:, wide : 2 * wide], pre[:, 3 * wide :]], axis=1)
    sig = jax.nn.sigmoid(pre_gate)
    silu = pre_gate * sig
    act = (silu * pre_up).astype(BF16).astype(F32)
    act_grad = weight * grad
    gate_b = (act_grad * pre_up * sig * (1.0 + pre_gate * (1.0 - sig))).astype(BF16)
    up_b = (act_grad * silu).astype(BF16)
    both = jnp.concatenate([gate_b[:, :wide], up_b[:, :wide], gate_b[:, wide:], up_b[:, wide:]], axis=1)
    thin_ref[:, : 2 * wide] = (both[:, : 2 * wide].astype(F32) * back_x).astype(BF16)
    thin_ref[:, 2 * wide :] = (act * weight * back_dy)[:, :wide].astype(BF16)
    hi, lo = split(act * grad)
    ones = (iota((16, 2 * wide), 0) == iota((16, 2 * wide), 1) % wide // (wide // 2)).astype(BF16)
    sums = dot(ones, hi.astype(BF16), 1, 1) + dot(ones, lo.astype(BF16), 1, 1)
    lines = jnp.concatenate(four(sums[0:1], sums[1:2]), axis=0)
    lines = jnp.concatenate([lines[:, :share], lines[:, share:]], axis=0).astype(BF16)
    for x in range(0, tps // 2, 2):
        at = [pl.ds(pl.multiple_of((2 * (x + i) + c_ref[0]) * share, share), share) for i in range(2)]
        dx = dot(both, jnp.concatenate([in_ref[:, a] for a in at], axis=1))
        for i in range(2):
            out_ref[x + i, :slots, :] = dx[:, i * share : i * share + share].astype(BF16)
            out_ref[x + i, slots:, :] = lines


def gather_up(blocks_ref, out_ref, *, cap):
    xs, tall, share = blocks_ref.shape
    slots = tall - 8
    total = blocks_ref[0].astype(F32)
    for x in range(1, xs):
        total = total + blocks_ref[x].astype(F32)
    dx = total[:slots].astype(BF16)
    lines = jnp.concatenate([total[slots : slots + 4], total[slots + 4 :]], axis=1)
    lines = four(lines[0:1] + lines[2:3], lines[1:2] + lines[3:4])
    lines = jnp.concatenate(lines + [jnp.zeros((share - 4, slots), F32)], axis=0).astype(BF16)
    row, slot = iota((out_ref.shape[0], slots), 0), iota((1, slots), 1)
    at = slot // cap * TILE + slot % cap
    out = dot((row == at).astype(BF16), dx) + dot((row == at + cap).astype(BF16), lines, 1, 1)
    out_ref[...] = out.astype(BF16)


def settle(target_ref, within_ref, home_ref, out_ref, gate_ref, *, cap):
    rows = out_ref.shape[0]
    row = iota((home_ref.shape[0], rows), 0)
    target = target_ref[...]
    home = home_ref[...]
    out_ref[...] = dot((row == target).astype(BF16), home, 0, 0).astype(BF16)
    dense = dot(home, (row == target + cap).astype(BF16), 0, 0)
    first = dense[0:1] + dense[2:3]
    second = dense[1:2] + dense[3:4]
    gate_ref[...] = jnp.where(within_ref[...] == 0, first, second)


def weights(full_ref, thin_ref, gate_ref, up_ref, down_ref):
    tps, slots, two = full_ref.shape
    share = two // 2
    wide = gate_ref.shape[0]
    for k in range(0, tps, 2):
        cols = slice(k * share, (k + 2) * share)
        x = jnp.concatenate([full_ref[k, :, :share], full_ref[k + 1, :, :share]], axis=1)
        dy = jnp.concatenate([full_ref[k, :, share:], full_ref[k + 1, :, share:]], axis=1)
        both = dot(thin_ref[:, : 2 * wide], x, 0, 0).astype(BF16)
        gate_ref[:, cols] = both[:wide]
        up_ref[:, cols] = both[wide:]
        down_ref[:, cols] = dot(thin_ref[:, 2 * wide :], dy, 0, 0).astype(BF16)


def on_device(tokens, cotangent, group_ids, within_ids, gate_weights, w_gate, w_up, w_down):
    eps = lax.axis_size("ep")
    xs, cs = lax.axis_size("x"), lax.axis_size("c")
    tps = xs * cs
    rows, width = tokens.shape
    count, _, hidden = w_gate.shape
    wide = count * hidden
    cap = (3 * rows + 2 * eps - 1) // (2 * eps)
    slots = eps * cap
    share = width // tps
    c = lax.axis_index("c").astype(jnp.int32)
    tp1 = (lax.axis_index("x").astype(jnp.int32) * cs + c).reshape(1)
    mine = jnp.concatenate([jnp.swapaxes(w_gate, 1, 2), jnp.swapaxes(w_up, 1, 2), w_down]).reshape(3 * wide, width)
    within_t = within_ids.T

    sent, target = call(
        route,
        [shape(eps * TILE, 2 * share), shape(1, rows, dtype=jnp.int32)],
        tp1, group_ids.T, within_t, gate_weights.T, tokens, cotangent,
        smem=1, held=(1, 2, 3, 4, 5), room=58, eps=eps, cap=cap, share=share,
        scratch=[
            pltpu.VMEM((1, rows), jnp.int32), pltpu.VMEM((2, rows), jnp.int32), pltpu.VMEM((2, rows), BF16),
            pltpu.VMEM((rows, width), BF16), pltpu.VMEM((rows, width), BF16), pltpu.SemaphoreType.DMA((5,)),
        ],
    )
    got = swap(sent.reshape(eps, TILE, 2 * share), "ep")
    theirs = lax.ppermute(mine, "c", [(0, 1), (1, 0)])
    thin = got[:, :cap, :].reshape(slots, 2 * share).astype(F16)
    full = lax.all_gather(thin, ("x", "c")).astype(BF16)

    blocks, thin_b = call(
        experts,
        [shape(xs, slots + 8, share), shape(slots, 3 * wide)],
        c.reshape(1), full, got.reshape(eps * TILE, 2 * share), mine, theirs,
        smem=1, held=(3, 4), flops=10**9, cap=cap,
        scratch=[pltpu.VMEM((slots, width), BF16)] * 2
        + [pltpu.VMEM((4 * wide, width), BF16), pltpu.VMEM((2 * wide, width), BF16), pltpu.SemaphoreType.DMA((2, 6))],
    )
    blocks = swap(blocks, "x")
    (home,) = call(gather_up, [shape(eps * TILE, share)], blocks, cap=cap)
    thin_b, home = lax.optimization_barrier((thin_b, home))
    home = swap(home.reshape(eps, TILE, share), "ep").reshape(eps * TILE, share)
    tokens_grad, gate_grad = call(
        settle, [shape(rows, share), shape(2, rows, dtype=F32)], target, within_t, home, cap=cap
    )
    gate_g, up_g, down_g = call(weights, [shape(wide, width)] * 3, full, thin_b, flops=10**9)
    return (
        tokens_grad,
        gate_grad.T,
        jnp.swapaxes(gate_g.reshape(count, hidden, width), 1, 2),
        jnp.swapaxes(up_g.reshape(count, hidden, width), 1, 2),
        down_g.reshape(count, hidden, width),
    )


def solution(mesh):
    eps, tps = mesh.shape["ep"], mesh.shape["tp"]
    fine = Mesh(mesh.devices.reshape(eps, tps // 2, 2), ("ep", "x", "c"))
    tp = ("x", "c")
    rows = P("ep", None)
    in_specs = (rows, rows, rows, rows, rows, P("ep", None, tp), P("ep", None, tp), P("ep", tp, None))
    out_specs = (P("ep", tp), rows, P("ep", None, tp), P("ep", None, tp), P("ep", tp, None))
    return jax.shard_map(on_device, mesh=fine, in_specs=in_specs, out_specs=out_specs, check_vma=False)
```
